32 devices in a mesh: sp: 8 (over z, x), dp: 4 (over y, core).
Axes of the slice: x: 2, y: 2, z: 4, core: 2. Of those that a mesh axis runs over, the one named last changes fastest.
Arguments:
- normed_input: bfloat16 [2560, 2048], P('sp'), may hold values from -6 to 6
- out_grad: bfloat16 [2560, 2048], P('sp'), may hold values from -6 to 6
- value_weight: bfloat16 [2048, 1024], P(None, 'dp'), may hold values from -0.125 to 0.125
- gate_weight: bfloat16 [2048, 1024], P(None, 'dp'), may hold values from -0.125 to 0.125
- down_weight: bfloat16 [1024, 2048], P('dp'), may hold values from -0.1875 to 0.1875
- conv_kernel: float32 [31, 1024], P(None, 'dp'), may hold values from -5 to 5
- conv_bias: float32 [1024], P('dp'), may hold values from -3 to 3
- norm_gain: float32 [1024], P('dp'), may hold values from 0.1 to 1.9
- norm_shift: float32 [1024], P('dp'), may hold values from -3 to 3
Outputs:
- input_grad: bfloat16 [2560, 2048], P('sp')
- value_grad: float32 [2048, 1024], P('sp', 'dp')
- gate_grad: float32 [2048, 1024], P('sp', 'dp')
- down_grad: float32 [1024, 2048], P('dp', 'sp')
- kernel_grad: float32 [31, 1024], P(None, 'dp')
- bias_grad: float32 [1024], P('dp')
- gain_grad: float32 [1024], P('dp')
- shift_grad: float32 [1024], P('dp')
The draws below stay inside these ranges and needn't reach their ends.
All inputs are finite; a program needn't handle non-finite values.
Results may differ from the reference program's by a relative error of at most 0.006.
Values may be sent and summed in bfloat16 or wider, within the bound.
A program may use at most 64 MiB of HBM per device.

```python
import math
import jax
import jax.numpy as jnp
from jax import lax

D = 2048
C = 1024
KW = 31
TOKENS = 2560


def draw_conv_kernel(key, part):
    first, second = jax.random.split(jax.random.fold_in(key, 11))
    place = jnp.arange(C, dtype=jnp.float32) / C
    jitter = jax.random.uniform(first, (C,), jnp.float32, -0.25, 0.25)
    scale = jnp.exp(jnp.log(0.5) + jnp.log(10.0) * place + jitter)
    base = jnp.clip(jax.random.normal(second, (KW, C), jnp.float32), -4.0, 4.0)
    return base * scale[None, :] / math.sqrt(KW)


def draw_conv_bias(key, part):
    noise_key = jax.random.fold_in(key, 23)
    place = jnp.arange(C, dtype=jnp.float32) / C
    noise = jnp.clip(jax.random.normal(noise_key, (C,), jnp.float32), -4.0, 4.0)
    return -0.8 + 2.0 * place + 0.4 * noise


def strengthened(array, key, source, target, blocks, factor):
    def block_of(dim):
        return (jnp.arange(array.shape[dim]) // (array.shape[dim] // blocks)).reshape((-1,) + (1,) * (array.ndim - 1 - dim))

    one_side = jax.random.permutation(key, blocks)[block_of(target)]
    second = (block_of(target) + blocks // 2) % blocks
    return jnp.where((block_of(source) == one_side) | (block_of(source) == second), factor * array, array)


def steps_of(key, shape, shards, least, high):
    gain, own = 1.0, jax.random.fold_in(key, 6)
    for axis_at, blocks in shards:
        draws = jnp.exp(jax.random.uniform(jax.random.fold_in(own, axis_at), (blocks,), jnp.float32, least / len(shards), high / len(shards)))
        gain = gain * jnp.repeat(draws, shape[axis_at] // blocks).reshape([-1 if axis == axis_at else 1 for axis in range(len(shape))])
    return gain


def bell_draw(rng, shape, scale, bound, cuts=(), kind=jnp.bfloat16):
    values = scale * jax.random.normal(rng, shape, jnp.float32)
    if cuts:
        values = values * steps_of(rng, shape, cuts, -0.22, 0.18)
    return jnp.clip(values, -bound, bound).astype(kind)


def heavy_noise(own_key, extent, scale, most, pieces, heavy, kind=jnp.bfloat16):
    values = scale * jax.random.normal(own_key, extent, jnp.float32)
    if pieces:
        values = values * steps_of(own_key, extent, pieces, -0.22, 0.18)
    return jnp.clip(strengthened(values, jax.random.fold_in(own_key, 3), *heavy), -most, most).astype(kind)


def setup_inputs(seed: int = 0) -> dict:
    keys = jax.random.split(jax.random.key(seed), 10)
    normed_input = heavy_noise(keys[0], (TOKENS, D), 1.0, 6.0, ((0, 8),), (0, 1, 8, 2.0))
    out_grad = heavy_noise(keys[1], (TOKENS, D), 1.0, 6.0, ((0, 8),), (0, 1, 8, 2.0))
    value_weight = bell_draw(keys[2], (D, C), D ** -0.5, 0.125, ((1, 4),))
    gate_weight = bell_draw(keys[3], (D, C), D ** -0.5, 0.125, ((1, 4),))
    down_weight = bell_draw(keys[4], (C, D), C ** -0.5, 0.1875, ((0, 4),))
    conv_kernel = draw_conv_kernel(jax.random.fold_in(keys[9], 71), 0)
    conv_bias = draw_conv_bias(jax.random.fold_in(keys[9], 71), 0)
    norm_gain = jnp.clip(1.0 + 0.18 * jax.random.normal(keys[7], (C,), jnp.float32), 0.1, 1.9)
    norm_shift = bell_draw(keys[8], (C,), 0.5, 3.0, ((0, 4),), jnp.float32)
    return {"normed_input": normed_input, "out_grad": out_grad, "value_weight": value_weight, "gate_weight": gate_weight, "down_weight": down_weight, "conv_kernel": conv_kernel, "conv_bias": conv_bias, "norm_gain": norm_gain, "norm_shift": norm_shift}


EPS = 1e-05

def reference(normed_input, out_grad, value_weight, gate_weight, down_weight, conv_kernel, conv_bias, norm_gain, norm_shift):
    reach = KW // 2
    ratio = 1.0 / math.sqrt(TOKENS)
    value_b = jnp.dot(normed_input, value_weight, preferred_element_type=jnp.float32).astype(jnp.bfloat16)
    gate_b = jnp.dot(normed_input, gate_weight, preferred_element_type=jnp.float32).astype(jnp.bfloat16)
    value = lax.optimization_barrier(value_b).astype(jnp.float32)
    gate = lax.optimization_barrier(gate_b).astype(jnp.float32)
    opening = jax.nn.sigmoid(gate)
    glu = value * opening
    padded = jnp.pad(glu, ((reach, reach), (0, 0)))
    mixed = jnp.zeros_like(glu) + conv_bias[None, :]
    for tap in range(KW):
        mixed = mixed + conv_kernel[tap][None, :] * padded[tap:tap + TOKENS]
    mean = lax.optimization_barrier(jnp.mean(mixed, axis=1, keepdims=True))
    spread = lax.optimization_barrier(jnp.mean((mixed - mean) * (mixed - mean), axis=1, keepdims=True))
    inv_std = lax.rsqrt(spread + EPS)
    centred = (mixed - mean) * inv_std
    normed = centred * norm_gain[None, :] + norm_shift[None, :]
    sig = jax.nn.sigmoid(normed)
    activated = (normed * sig).astype(jnp.bfloat16)
    d_act = jnp.dot(out_grad, down_weight.T, preferred_element_type=jnp.float32)
    d_normed = d_act * sig * (1.0 + normed * (1.0 - sig))
    d_centred = d_normed * norm_gain[None, :]
    first = lax.optimization_barrier(jnp.mean(d_centred, axis=1, keepdims=True))
    second = lax.optimization_barrier(jnp.mean(d_centred * centred, axis=1, keepdims=True))
    d_mixed = inv_std * (d_centred - first - centred * second)
    d_padded = jnp.pad(d_mixed, ((reach, reach), (0, 0)))
    d_glu = jnp.zeros_like(d_mixed)
    for tap in range(KW):
        d_glu = d_glu + conv_kernel[tap][None, :] * d_padded[2 * reach - tap:2 * reach - tap + TOKENS]
    kernel_grad = jnp.stack([lax.optimization_barrier(jnp.sum(d_mixed * padded[tap:tap + TOKENS], axis=0)) for tap in range(KW)]) * ratio
    bias_grad = lax.optimization_barrier(jnp.sum(d_mixed, axis=0)) * ratio
    gain_grad = lax.optimization_barrier(jnp.sum(d_normed * centred, axis=0)) * ratio
    shift_grad = lax.optimization_barrier(jnp.sum(d_normed, axis=0)) * ratio
    d_value = (d_glu * opening).astype(jnp.bfloat16)
    d_gate = (d_glu * value * opening * (1.0 - opening)).astype(jnp.bfloat16)
    value_grad = jnp.dot(normed_input.T, d_value, preferred_element_type=jnp.float32) * ratio
    gate_grad = jnp.dot(normed_input.T, d_gate, preferred_element_type=jnp.float32) * ratio
    down_grad = jnp.dot(activated.T, out_grad, preferred_element_type=jnp.float32) * ratio
    input_grad = (jnp.dot(d_value, value_weight.T, preferred_element_type=jnp.float32) + jnp.dot(d_gate, gate_weight.T, preferred_element_type=jnp.float32)).astype(jnp.bfloat16)
    return (input_grad, value_grad, gate_grad, down_grad, kernel_grad, bias_grad, gain_grad, shift_grad)
```

```python
import functools
import math

import jax
import jax.numpy as jnp
from jax import lax
from jax.experimental import pallas as pl
from jax.experimental.pallas import tpu as pltpu
from jax.sharding import PartitionSpec as P

EPS = 1e-05
F32 = jnp.float32
BF16 = jnp.bfloat16
MESH = pl.DeviceIdType.MESH
NT = (((1,), (1,)), ((), ()))
TN = (((0,), (0,)), ((), ()))
EXACT = lax.Precision.HIGHEST
PAD = 16
ROWS = 32


def dot(a, b, numbers, precision=None):
    return lax.dot_general(a, b, numbers, precision=precision, preferred_element_type=F32)


def kernel(
    sp,
    dp,
    ratio,
    x,
    og,
    wv,
    wg,
    wd,
    ck,
    bias,
    gain,
    shift,
    ig_out,
    vg_out,
    gg_out,
    dg_out,
    small_out,
    value,
    opening,
    glu,
    mixed,
    d_act,
    d_pad,
    act,
    dv,
    dg,
    cols,
    stats,
    stats2,
    part,
    ring_src,
    ring_dst,
    ig_send,
    ig_recv,
    ig_own,
    ig_sum,
    ig_peer,
    small,
    small_recv,
    halo_send,
    halo_recv,
    stat_send,
    stat_recv,
    ring_send,
    ring_recv,
    ig_ssem,
    ig_rsem,
    small_ssem,
    small_rsem,
):
    tokens, width = x.shape
    taps, chans = ck.shape
    channels = chans * dp
    reach = taps // 2
    chunk = width // sp
    half_chunk = chunk // 2
    tile = min(256, width)
    s = lax.axis_index("sp")
    d = lax.axis_index("dp")
    bits_sp = sp.bit_length() - 1
    bits_dp = dp.bit_length() - 1

    def flip(i, bit):
        step = 1 << bit
        return i + step * (1 - 2 * lax.rem(lax.div(i, step), 2))

    def index_of(p):
        far = lax.div(p, sp // 2)
        return (1 - far) * 2 * p + far * (2 * sp - 1 - 2 * p)

    odd = lax.rem(s, 2)
    pos = (1 - odd) * lax.div(s, 2) + odd * (sp - 1 - lax.div(s, 2))
    ahead = index_of(lax.rem(pos + 1, sp))
    behind = index_of(lax.rem(pos + sp - 1, sp))

    barrier = pltpu.get_barrier_semaphore()
    peers = [ahead, behind, lax.rem(s + 1, sp), lax.rem(s + sp - 1, sp)]
    peers += [flip(s, bit) for bit in range(bits_sp)]
    for peer in peers:
        pl.semaphore_signal(barrier, inc=1, device_id={"sp": peer}, device_id_type=MESH)
    for off in range(1, dp):
        pl.semaphore_signal(
            barrier, inc=1, device_id={"dp": lax.rem(d + off, dp)}, device_id_type=MESH
        )

    numbers = (((1,), (0,)), ((), ()))
    value[...] = dot(x[...], wv[...], numbers).astype(BF16).astype(F32)
    opening[...] = dot(x[...], wg[...], numbers).astype(BF16).astype(F32)

    def row_loop(fn, init=None, rows=ROWS):
        def step(i, carry):
            return fn(pl.multiple_of(i * rows, rows), carry)

        return lax.fori_loop(0, tokens // rows, step, init)

    def make_glu(r, _):
        here = pl.ds(r, ROWS)
        o = jax.nn.sigmoid(opening[here, :])
        opening[here, :] = o
        glu[pl.ds(r + PAD, ROWS), :] = value[here, :] * o

    row_loop(make_glu)
    pl.semaphore_wait(barrier, len(peers) + dp - 1)

    has_low, has_high = s > 0, s < sp - 1

    def halo_copies(buf, at):
        up = pltpu.make_async_remote_copy(
            src_ref=buf.at[pl.ds(tokens, PAD)],
            dst_ref=buf.at[pl.ds(0, PAD)],
            send_sem=halo_send.at[at],
            recv_sem=halo_recv.at[at],
            device_id={"sp": lax.rem(s + 1, sp)},
            device_id_type=MESH,
        )
        down = pltpu.make_async_remote_copy(
            src_ref=buf.at[pl.ds(PAD, PAD)],
            dst_ref=buf.at[pl.ds(tokens + PAD, PAD)],
            send_sem=halo_send.at[at + 1],
            recv_sem=halo_recv.at[at + 1],
            device_id={"sp": lax.rem(s + sp - 1, sp)},
            device_id_type=MESH,
        )
        return up, down

    def halo_start(buf, at):
        up, down = halo_copies(buf, at)
        pl.when(has_high)(up.start)
        pl.when(has_low)(down.start)

        @pl.when(s == 0)
        def _():
            buf[pl.ds(0, PAD), :] = jnp.zeros((PAD, chans), F32)

        @pl.when(s == sp - 1)
        def _():
            buf[pl.ds(tokens + PAD, PAD), :] = jnp.zeros((PAD, chans), F32)

    def halo_wait(buf, at):
        up, down = halo_copies(buf, at)

        @pl.when(has_low)
        def _():
            up.wait_recv()
            down.wait_send()

        @pl.when(has_high)
        def _():
            down.wait_recv()
            up.wait_send()

    halo_start(glu, 0)
    d_act[...] = dot(og[...], wd[...], NT)
    halo_wait(glu, 0)

    span = ROWS + 2 * PAD

    def shifted(buf, r, offset):
        window = buf[pl.ds(r, span), :]
        return pltpu.roll(window, span - offset, 0) if offset else window

    def slide(buf, r, offset_of, acc):
        for low in range(8):
            those = [tap for tap in range(taps) if offset_of(tap) % 8 == low]
            if those:
                window = shifted(buf, r, low)
                for tap in those:
                    high = offset_of(tap) - low
                    acc = acc + ck[tap : tap + 1, :] * window[high : high + ROWS]
        return acc

    def conv(r, _):
        acc = jnp.zeros((ROWS, chans), F32) + bias[...]
        mixed[pl.ds(r, ROWS), :] = slide(glu, r, lambda tap: tap + PAD - reach, acc)

    row_loop(conv)

    ones = jnp.ones((8, chans), F32)
    line = lax.broadcasted_iota(jnp.int32, (8, tokens), 0)
    eye = (
        lax.broadcasted_iota(jnp.int32, (8, 128), 0)
        == lax.broadcasted_iota(jnp.int32, (8, 128), 1)
    ).astype(F32)

    def stat_copy(buf, off, at):
        return pltpu.make_async_remote_copy(
            src_ref=buf.at[0],
            dst_ref=buf.at[off],
            send_sem=stat_send.at[at * dp + off],
            recv_sem=stat_recv.at[at * dp + off],
            device_id={"dp": lax.rem(d + off, dp)},
            device_id_type=MESH,
        )

    def stat_start(buf, at, one, two):
        buf[0] = jnp.where(line == 0, dot(ones, one, NT, EXACT), dot(ones, two, NT, EXACT))
        for off in range(1, dp):
            stat_copy(buf, off, at).start()

    def stat_wait(buf, at):
        for off in range(1, dp):
            stat_copy(buf, off, at).wait()
        total = buf[0]
        for off in range(1, dp):
            total = total + buf[off]
        return total * (1.0 / channels)

    stat_start(stats, 0, mixed[...], mixed[...] * mixed[...])
    moments = stat_wait(stats, 0)
    mean = moments[0:1]
    inv = lax.rsqrt(moments[1:2] - mean * mean + EPS)
    cols[0] = dot(jnp.where(line == 0, mean, inv), eye, TN, EXACT)

    def norm(r, carry):
        gain_sum, shift_sum = carry
        here = pl.ds(r, ROWS)
        col = cols[0, here, :]
        centred = (mixed[here, :] - col[:, 0:1]) * col[:, 1:2]
        normed = centred * gain[...] + shift[...]
        sig = jax.nn.sigmoid(normed)
        act[here, :] = (normed * sig).astype(BF16)
        d_normed = d_act[here, :] * sig * (1.0 + normed * (1.0 - sig))
        mixed[here, :] = centred
        d_act[here, :] = d_normed * gain[...]
        gain_sum = gain_sum + jnp.sum(d_normed * centred, axis=0, keepdims=True)
        shift_sum = shift_sum + jnp.sum(d_normed, axis=0, keepdims=True)
        return gain_sum, shift_sum

    zero = jnp.zeros((1, chans), F32)
    gain_sum, shift_sum = row_loop(norm, (zero, zero))
    stat_start(stats2, 1, d_act[...], d_act[...] * mixed[...])

    def weight_grad(at, rows, factor):
        def step(i, _):
            here = pl.ds(pl.multiple_of(i * tile, tile), tile)
            part[at, here, :] = dot(rows[:, here], factor[...], TN) * ratio

        lax.fori_loop(0, width // tile, step, None)

    streams = [(0, 0, 1), (1, 0, -1), (0, 1, 1), (1, 1, -1), (2, 0, 1), (2, 1, -1)]
    late, early = (0, 1, 2, 3), (4, 5)

    def piece(stream, p):
        at, half, _ = streams[stream]
        first = index_of(lax.rem(p + 2 * sp, sp)) * chunk + half * half_chunk
        return part[at, pl.ds(pl.multiple_of(first, half_chunk), half_chunk), :]

    def ring_copy(stream, k):
        return pltpu.make_async_remote_copy(
            src_ref=ring_src.at[stream, k],
            dst_ref=ring_dst.at[stream, k],
            send_sem=ring_send.at[stream, k],
            recv_sem=ring_recv.at[stream, k],
            device_id={"sp": ahead if streams[stream][2] == 1 else behind},
            device_id_type=MESH,
        )

    def ring_step(k, which):
        for stream in which:
            way = streams[stream][2]
            mine = piece(stream, pos - way * (1 + k))
            if not (isinstance(k, int) and k == 0):
                ring_copy(stream, k - 1).wait_recv()
                mine = mine + ring_dst[stream, k - 1].astype(F32)
            ring_src[stream, k] = mine.astype(BF16)
            ring_copy(stream, k).start()

    def ring_end(which, outs):
        for stream in which:
            at, half, _ = streams[stream]
            ring_copy(stream, sp - 2).wait_recv()
            outs[at][pl.ds(half * half_chunk, half_chunk), :] = piece(stream, pos) + ring_dst[
                stream, sp - 2
            ].astype(F32)

    weight_grad(2, og, act)
    ring_step(0, early)

    moments = stat_wait(stats2, 1)
    cols[1] = dot(moments, eye, TN, EXACT)

    def norm_back(r, bias_sum):
        here = pl.ds(r, ROWS)
        col, back = cols[0, here, :], cols[1, here, :]
        d_mixed = col[:, 1:2] * (d_act[here, :] - back[:, 0:1] - mixed[here, :] * back[:, 1:2])
        d_pad[pl.ds(r + PAD, ROWS), :] = d_mixed
        return bias_sum + jnp.sum(d_mixed, axis=0, keepdims=True)

    bias_sum = row_loop(norm_back, zero)
    halo_start(d_pad, 2)

    small[0] = jnp.zeros(small.shape[1:], F32)
    for low in range(0, 8, 2):
        those = [
            [tap for tap in range(taps) if (tap + PAD - reach) % 8 == low + at] for at in range(2)
        ]

        def taps_sum(r, sums, low=low, those=those):
            grad = d_pad[pl.ds(r + PAD, ROWS), :]
            new = []
            for at in range(2):
                window = shifted(glu, r, low + at)
                for tap in those[at]:
                    high = tap + PAD - reach - low - at
                    prod = grad * window[high : high + ROWS]
                    acc = sums[len(new)]
                    for row in range(0, ROWS, 8):
                        acc = acc + prod[row : row + 8]
                    new.append(acc)
            return tuple(new)

        flat = those[0] + those[1]
        sums = row_loop(taps_sum, tuple(jnp.zeros((8, chans), F32) for _ in flat))
        for acc, tap in zip(sums, flat):
            small[0, tap : tap + 1, :] = jnp.sum(acc, axis=0, keepdims=True) * ratio
        if low == 2:
            ring_step(1, early)
    small[0, taps : taps + 1, :] = bias_sum * ratio
    small[0, taps + 1 : taps + 2, :] = gain_sum * ratio
    small[0, taps + 2 : taps + 3, :] = shift_sum * ratio

    def small_copy(bit):
        return pltpu.make_async_remote_copy(
            src_ref=small.at[bit],
            dst_ref=small_recv.at[bit],
            send_sem=small_ssem.at[bit],
            recv_sem=small_rsem.at[bit],
            device_id={"sp": flip(s, bit)},
            device_id_type=MESH,
        )

    def small_next(bit):
        small_copy(bit).wait_recv()
        return small[bit] + small_recv[bit]

    halo_wait(d_pad, 2)
    small_copy(0).start()

    def conv_back(r, _):
        here = pl.ds(r, ROWS)
        acc = jnp.zeros((ROWS, chans), F32)
        acc = slide(d_pad, r, lambda tap: PAD + reach - tap, acc)
        o = opening[here, :]
        grad = acc * o
        dv[here, :] = grad.astype(BF16)
        dg[here, :] = (grad * value[here, :] * (1.0 - o)).astype(BF16)

    row_loop(conv_back)
    weight_grad(0, x, dv)
    ring_step(0, late[0::2])
    weight_grad(1, x, dg)
    ring_step(0, late[1::2])
    ring_step(2, early)

    half = tokens // 2
    mine = pl.multiple_of(lax.rem(d, 2) * half, half)
    other = pl.multiple_of((1 - lax.rem(d, 2)) * half, half)

    def input_grad(first, target):
        def step(i, _):
            here = pl.ds(pl.multiple_of(i * tile, tile), tile)
            rows = pl.ds(first, half)
            got = dot(dv[rows, :], wv[here, :], NT) + dot(dg[rows, :], wg[here, :], NT)
            target[:, here] = got.astype(target.dtype)

        lax.fori_loop(0, width // tile, step, None)

    def ig_copy(at, src, dst, bit):
        return pltpu.make_async_remote_copy(
            src_ref=src,
            dst_ref=dst,
            send_sem=ig_ssem.at[at],
            recv_sem=ig_rsem.at[at],
            device_id={"dp": flip(d, bit)},
            device_id_type=MESH,
        )

    input_grad(other, ig_send)
    copy0 = ig_copy(0, ig_send, ig_recv, 0)
    copy0.start()
    input_grad(mine, ig_own)
    copy0.wait_recv()

    def wide_loop(fn):
        def step(i, _):
            fn(pl.ds(pl.multiple_of(i * tile, tile), tile))

        lax.fori_loop(0, width // tile, step, None)

    def pair_sum(here):
        ig_sum[0, :, here] = (ig_own[:, here] + ig_recv[:, here].astype(F32)).astype(BF16)

    def y_copy(bit):
        return ig_copy(bit, ig_sum.at[bit - 1], ig_peer.at[bit - 1], bit)

    wide_loop(pair_sum)
    last = bits_dp
    if last > 1:
        y_copy(1).start()
    small[1] = small_next(0)
    if bits_sp > 1:
        small_copy(1).start()

    everything = late + early
    ring_step(1, late)
    ring_step(3, early) if sp > 4 else None
    ring_step(2, late)
    for bit in range(1, bits_sp):
        small[bit + 1] = small_next(bit)
        if bit + 1 < bits_sp:
            small_copy(bit + 1).start()
    ring_step(3, late)

    for_early = 4

    def both(k, _):
        ring_step(k, everything)

    lax.fori_loop(for_early, sp - 2, both, None)

    for bit in range(1, bits_dp):
        y_copy(bit).wait_recv()

        def add(here, bit=bit):
            got = ig_sum[bit - 1, :, here].astype(F32) + ig_peer[bit - 1, :, here].astype(F32)
            ig_sum[bit, :, here] = got.astype(BF16)

        wide_loop(add)
        if bit + 1 < bits_dp:
            y_copy(bit + 1).start()

    final = bits_dp - 1
    give = ig_copy(
        bits_dp, ig_sum.at[final], ig_out.at[pl.ds(mine, half)], 0
    )
    give.start()
    ring_step(sp - 2, everything)

    def keep(here):
        ig_out[pl.ds(mine, half), here] = ig_sum[final, :, here]

    wide_loop(keep)
    small_out[...] = small[bits_sp]
    outs = (vg_out, gg_out, dg_out)
    ring_end(everything, outs)

    copy0.wait_send()
    for bit in range(1, bits_dp):
        y_copy(bit).wait_send()
    give.wait()
    for bit in range(bits_sp):
        small_copy(bit).wait_send()

    def drain(k, _):
        for stream in everything:
            ring_copy(stream, k).wait_send()

    lax.fori_loop(0, sp - 1, drain, None)


def on_device(
    normed_input,
    out_grad,
    value_weight,
    gate_weight,
    down_weight,
    conv_kernel,
    conv_bias,
    norm_gain,
    norm_shift,
):
    tokens, width = normed_input.shape
    taps, chans = conv_kernel.shape
    sp, dp = lax.axis_size("sp"), lax.axis_size("dp")
    ratio = 1.0 / math.sqrt(tokens * sp)
    chunk = width // sp
    bits_sp, bits_dp = sp.bit_length() - 1, dp.bit_length() - 1
    small_rows = -(-(taps + 3) // 8) * 8
    half = tokens // 2
    full = (tokens, chans)
    vmem = pl.BlockSpec(memory_space=pltpu.VMEM)
    dma = pltpu.SemaphoreType.DMA
    ig, vg, gg, dgrad, small = pl.pallas_call(
        functools.partial(kernel, sp, dp, ratio),
        out_shape=(
            jax.ShapeDtypeStruct((tokens, width), BF16),
            jax.ShapeDtypeStruct((chunk, chans), F32),
            jax.ShapeDtypeStruct((chunk, chans), F32),
            jax.ShapeDtypeStruct((chunk, chans), F32),
            jax.ShapeDtypeStruct((small_rows, chans), F32),
        ),
        in_specs=[vmem] * 9,
        out_specs=(vmem,) * 5,
        scratch_shapes=[
            pltpu.VMEM(full, F32),
            pltpu.VMEM(full, F32),
            pltpu.VMEM((tokens + 2 * PAD, chans), F32),
            pltpu.VMEM(full, F32),
            pltpu.VMEM(full, F32),
            pltpu.VMEM((tokens + 2 * PAD, chans), F32),
            pltpu.VMEM(full, BF16),
            pltpu.VMEM(full, BF16),
            pltpu.VMEM(full, BF16),
            pltpu.VMEM((2, tokens, 128), F32),
            pltpu.VMEM((dp, 8, tokens), F32),
            pltpu.VMEM((dp, 8, tokens), F32),
            pltpu.VMEM((3, width, chans), F32),
            pltpu.VMEM((6, sp - 1, chunk // 2, chans), BF16),
            pltpu.VMEM((6, sp - 1, chunk // 2, chans), BF16),
            pltpu.VMEM((half, width), BF16),
            pltpu.VMEM((half, width), BF16),
            pltpu.VMEM((half, width), F32),
            pltpu.VMEM((bits_dp, half, width), BF16),
            pltpu.VMEM((bits_dp - 1, half, width), BF16),
            pltpu.VMEM((bits_sp + 1, small_rows, chans), F32),
            pltpu.VMEM((bits_sp, small_rows, chans), F32),
            dma((4,)),
            dma((4,)),
            dma((2 * dp,)),
            dma((2 * dp,)),
            dma((6, sp - 1)),
            dma((6, sp - 1)),
            dma((bits_dp + 1,)),
            dma((bits_dp + 1,)),
            dma((bits_sp,)),
            dma((bits_sp,)),
        ],
        compiler_params=pltpu.CompilerParams(
            collective_id=0, has_side_effects=True, vmem_limit_bytes=60 * 1024 * 1024
        ),
    )(
        normed_input,
        out_grad,
        value_weight,
        gate_weight,
        down_weight,
        conv_kernel,
        conv_bias[None, :],
        norm_gain[None, :],
        norm_shift[None, :],
    )
    return (
        ig,
        vg,
        gg,
        dgrad.T,
        small[:taps],
        small[taps],
        small[taps + 1],
        small[taps + 2],
    )


def solution(mesh):
    in_specs = (
        P("sp", None),
        P("sp", None),
        P(None, "dp"),
        P(None, "dp"),
        P("dp", None),
        P(None, "dp"),
        P("dp"),
        P("dp"),
        P("dp"),
    )
    out_specs = (
        P("sp", None),
        P("sp", "dp"),
        P("sp", "dp"),
        P("dp", "sp"),
        P(None, "dp"),
        P("dp"),
        P("dp"),
        P("dp"),
    )
    return jax.shard_map(
        on_device, mesh=mesh, in_specs=in_specs, out_specs=out_specs, check_vma=False
    )
```

```python
import functools
import math

import jax
import jax.numpy as jnp
from jax import lax
from jax.experimental import pallas as pl
from jax.experimental.pallas import tpu as pltpu
from jax.sharding import PartitionSpec as P

EPS = 1e-05
F32 = jnp.float32
BF16 = jnp.bfloat16
MESH = pl.DeviceIdType.MESH
NT = (((1,), (1,)), ((), ()))
TN = (((0,), (0,)), ((), ()))
EXACT = lax.Precision.HIGHEST
PAD = 16
ROWS = 32
MAIN = 61_900_000
FINISH = 16_000_000


def dot(a, b, numbers, precision=None):
    return lax.dot_general(a, b, numbers, precision=precision, preferred_element_type=F32)


def kernel(
    sp,
    dp,
    ratio,
    x_hbm,
    og_hbm,
    wv_hbm,
    wg_hbm,
    wd_hbm,
    ck,
    bias,
    gain,
    shift,
    ig_out,
    vg_out,
    gg_out,
    dg_out,
    small_out,
    x,
    og,
    wv,
    wg,
    wd,
    load_sem,
    value,
    opening,
    glu,
    mixed,
    d_act,
    d_pad,
    act,
    dv,
    dg,
    cols,
    stats,
    stats2,
    part,
    ring_src,
    ring_dst,
    ig_send,
    ig_recv,
    ig_own,
    ig_sum,
    ig_peer,
    small,
    small_recv,
    halo_send,
    halo_recv,
    stat_send,
    stat_recv,
    ring_send,
    ring_recv,
    ig_ssem,
    ig_rsem,
    small_ssem,
    small_rsem,
):
    tokens, width = x.shape
    taps, chans = ck.shape
    channels = chans * dp
    reach = taps // 2
    chunk = width // sp
    half_chunk = chunk // 2
    tile = min(256, width)
    s = lax.axis_index("sp")
    d = lax.axis_index("dp")
    bits_sp = sp.bit_length() - 1
    bits_dp = dp.bit_length() - 1

    def flip(i, bit):
        step = 1 << bit
        return i + step * (1 - 2 * lax.rem(lax.div(i, step), 2))

    def index_of(p):
        far = lax.div(p, sp // 2)
        return (1 - far) * 2 * p + far * (2 * sp - 1 - 2 * p)

    odd = lax.rem(s, 2)
    pos = (1 - odd) * lax.div(s, 2) + odd * (sp - 1 - lax.div(s, 2))
    ahead = index_of(lax.rem(pos + 1, sp))
    behind = index_of(lax.rem(pos + sp - 1, sp))

    loads = [
        pltpu.make_async_copy(src, dst, load_sem.at[at])
        for at, (src, dst) in enumerate(
            [(x_hbm, x), (wv_hbm, wv), (wg_hbm, wg), (og_hbm, og), (wd_hbm, wd)]
        )
    ]
    for load in loads:
        load.start()

    barrier = pltpu.get_barrier_semaphore()
    peers = [ahead, behind, lax.rem(s + 1, sp), lax.rem(s + sp - 1, sp)]
    peers += [flip(s, bit) for bit in range(bits_sp)]
    for peer in peers:
        pl.semaphore_signal(barrier, inc=1, device_id={"sp": peer}, device_id_type=MESH)
    for off in range(1, dp):
        pl.semaphore_signal(
            barrier, inc=1, device_id={"dp": lax.rem(d + off, dp)}, device_id_type=MESH
        )

    numbers = (((1,), (0,)), ((), ()))
    loads[0].wait()
    loads[1].wait()
    value[...] = dot(x[...], wv[...], numbers).astype(BF16).astype(F32)
    loads[2].wait()
    opening[...] = dot(x[...], wg[...], numbers).astype(BF16).astype(F32)

    def row_loop(fn, init=None, rows=ROWS):
        def step(i, carry):
            return fn(pl.multiple_of(i * rows, rows), carry)

        return lax.fori_loop(0, tokens // rows, step, init)

    def make_glu(r, _):
        here = pl.ds(r, ROWS)
        o = jax.nn.sigmoid(opening[here, :])
        opening[here, :] = o
        glu[pl.ds(r + PAD, ROWS), :] = value[here, :] * o

    row_loop(make_glu)
    pl.semaphore_wait(barrier, len(peers) + dp - 1)

    has_low, has_high = s > 0, s < sp - 1

    def halo_copies(buf, at):
        up = pltpu.make_async_remote_copy(
            src_ref=buf.at[pl.ds(tokens, PAD)],
            dst_ref=buf.at[pl.ds(0, PAD)],
            send_sem=halo_send.at[at],
            recv_sem=halo_recv.at[at],
            device_id={"sp": lax.rem(s + 1, sp)},
            device_id_type=MESH,
        )
        down = pltpu.make_async_remote_copy(
            src_ref=buf.at[pl.ds(PAD, PAD)],
            dst_ref=buf.at[pl.ds(tokens + PAD, PAD)],
            send_sem=halo_send.at[at + 1],
            recv_sem=halo_recv.at[at + 1],
            device_id={"sp": lax.rem(s + sp - 1, sp)},
            device_id_type=MESH,
        )
        return up, down

    def halo_start(buf, at):
        up, down = halo_copies(buf, at)
        pl.when(has_high)(up.start)
        pl.when(has_low)(down.start)

        @pl.when(s == 0)
        def _():
            buf[pl.ds(0, PAD), :] = jnp.zeros((PAD, chans), F32)

        @pl.when(s == sp - 1)
        def _():
            buf[pl.ds(tokens + PAD, PAD), :] = jnp.zeros((PAD, chans), F32)

    def halo_wait(buf, at):
        up, down = halo_copies(buf, at)

        @pl.when(has_low)
        def _():
            up.wait_recv()
            down.wait_send()

        @pl.when(has_high)
        def _():
            down.wait_recv()
            up.wait_send()

    halo_start(glu, 0)
    loads[3].wait()
    loads[4].wait()
    d_act[...] = dot(og[...], wd[...], NT)
    halo_wait(glu, 0)

    span = ROWS + 2 * PAD

    def shifted(buf, r, offset):
        window = buf[pl.ds(r, span), :]
        return pltpu.roll(window, span - offset, 0) if offset else window

    def slide(buf, r, offset_of, acc):
        for low in range(8):
            those = [tap for tap in range(taps) if offset_of(tap) % 8 == low]
            if those:
                window = shifted(buf, r, low)
                for tap in those:
                    high = offset_of(tap) - low
                    acc = acc + ck[tap : tap + 1, :] * window[high : high + ROWS]
        return acc

    def conv(r, _):
        acc = jnp.zeros((ROWS, chans), F32) + bias[...]
        mixed[pl.ds(r, ROWS), :] = slide(glu, r, lambda tap: tap + PAD - reach, acc)

    row_loop(conv)

    ones = jnp.ones((8, chans), F32)
    line = lax.broadcasted_iota(jnp.int32, (8, tokens), 0)
    eye = (
        lax.broadcasted_iota(jnp.int32, (8, 128), 0)
        == lax.broadcasted_iota(jnp.int32, (8, 128), 1)
    ).astype(F32)

    def stat_copy(buf, off, at):
        return pltpu.make_async_remote_copy(
            src_ref=buf.at[0],
            dst_ref=buf.at[off],
            send_sem=stat_send.at[at * dp + off],
            recv_sem=stat_recv.at[at * dp + off],
            device_id={"dp": lax.rem(d + off, dp)},
            device_id_type=MESH,
        )

    def stat_start(buf, at, one, two):
        buf[0] = jnp.where(line == 0, dot(ones, one, NT, EXACT), dot(ones, two, NT, EXACT))
        for off in range(1, dp):
            stat_copy(buf, off, at).start()

    def stat_wait(buf, at):
        for off in range(1, dp):
            stat_copy(buf, off, at).wait()
        total = buf[0]
        for off in range(1, dp):
            total = total + buf[off]
        return total * (1.0 / channels)

    stat_start(stats, 0, mixed[...], mixed[...] * mixed[...])
    moments = stat_wait(stats, 0)
    mean = moments[0:1]
    inv = lax.rsqrt(moments[1:2] - mean * mean + EPS)
    cols[0] = dot(jnp.where(line == 0, mean, inv), eye, TN, EXACT)

    def norm(r, carry):
        gain_sum, shift_sum = carry
        here = pl.ds(r, ROWS)
        col = cols[0, here, :]
        centred = (mixed[here, :] - col[:, 0:1]) * col[:, 1:2]
        normed = centred * gain[...] + shift[...]
        sig = jax.nn.sigmoid(normed)
        act[here, :] = (normed * sig).astype(BF16)
        d_normed = d_act[here, :] * sig * (1.0 + normed * (1.0 - sig))
        mixed[here, :] = centred
        d_act[here, :] = d_normed * gain[...]
        gain_sum = gain_sum + jnp.sum(d_normed * centred, axis=0, keepdims=True)
        shift_sum = shift_sum + jnp.sum(d_normed, axis=0, keepdims=True)
        return gain_sum, shift_sum

    zero = jnp.zeros((1, chans), F32)
    gain_sum, shift_sum = row_loop(norm, (zero, zero))
    stat_start(stats2, 1, d_act[...], d_act[...] * mixed[...])

    def weight_grad(at, rows, factor):
        def step(i, _):
            here = pl.ds(pl.multiple_of(i * tile, tile), tile)
            part[at, here, :] = dot(rows[:, here], factor[...], TN) * ratio

        lax.fori_loop(0, width // tile, step, None)

    streams = [(0, 0, 1), (1, 0, -1), (0, 1, 1), (1, 1, -1), (2, 0, 1), (2, 1, -1)]
    late, early = (0, 1, 2, 3), (4, 5)

    def piece(stream, p):
        at, half, _ = streams[stream]
        first = index_of(lax.rem(p + 2 * sp, sp)) * chunk + half * half_chunk
        return part[at, pl.ds(pl.multiple_of(first, half_chunk), half_chunk), :]

    def ring_copy(stream, k):
        return pltpu.make_async_remote_copy(
            src_ref=ring_src.at[stream, k],
            dst_ref=ring_dst.at[stream, k],
            send_sem=ring_send.at[stream, k],
            recv_sem=ring_recv.at[stream, k],
            device_id={"sp": ahead if streams[stream][2] == 1 else behind},
            device_id_type=MESH,
        )

    def ring_step(k, which):
        for stream in which:
            way = streams[stream][2]
            mine = piece(stream, pos - way * (1 + k))
            if not (isinstance(k, int) and k == 0):
                ring_copy(stream, k - 1).wait_recv()
                mine = mine + ring_dst[stream, k - 1].astype(F32)
            ring_src[stream, k] = mine.astype(BF16)
            ring_copy(stream, k).start()

    def ring_end(which, outs):
        for stream in which:
            at, half, _ = streams[stream]
            ring_copy(stream, sp - 2).wait_recv()
            outs[at][pl.ds(half * half_chunk, half_chunk), :] = piece(stream, pos) + ring_dst[
                stream, sp - 2
            ].astype(F32)

    weight_grad(2, og, act)
    ring_step(0, early)

    moments = stat_wait(stats2, 1)
    cols[1] = dot(moments, eye, TN, EXACT)

    def norm_back(r, bias_sum):
        here = pl.ds(r, ROWS)
        col, back = cols[0, here, :], cols[1, here, :]
        d_mixed = col[:, 1:2] * (d_act[here, :] - back[:, 0:1] - mixed[here, :] * back[:, 1:2])
        d_pad[pl.ds(r + PAD, ROWS), :] = d_mixed
        return bias_sum + jnp.sum(d_mixed, axis=0, keepdims=True)

    bias_sum = row_loop(norm_back, zero)
    halo_start(d_pad, 2)

    small[0] = jnp.zeros(small.shape[1:], F32)
    for low in range(0, 8, 2):
        those = [
            [tap for tap in range(taps) if (tap + PAD - reach) % 8 == low + at] for at in range(2)
        ]

        def taps_sum(r, sums, low=low, those=those):
            grad = d_pad[pl.ds(r + PAD, ROWS), :]
            new = []
            for at in range(2):
                window = shifted(glu, r, low + at)
                for tap in those[at]:
                    high = tap + PAD - reach - low - at
                    prod = grad * window[high : high + ROWS]
                    acc = sums[len(new)]
                    for row in range(0, ROWS, 8):
                        acc = acc + prod[row : row + 8]
                    new.append(acc)
            return tuple(new)

        flat = those[0] + those[1]
        sums = row_loop(taps_sum, tuple(jnp.zeros((8, chans), F32) for _ in flat))
        for acc, tap in zip(sums, flat):
            small[0, tap : tap + 1, :] = jnp.sum(acc, axis=0, keepdims=True) * ratio
        if low == 2:
            ring_step(1, early)
    small[0, taps : taps + 1, :] = bias_sum * ratio
    small[0, taps + 1 : taps + 2, :] = gain_sum * ratio
    small[0, taps + 2 : taps + 3, :] = shift_sum * ratio

    def small_copy(bit):
        return pltpu.make_async_remote_copy(
            src_ref=small.at[bit],
            dst_ref=small_recv.at[bit],
            send_sem=small_ssem.at[bit],
            recv_sem=small_rsem.at[bit],
            device_id={"sp": flip(s, bit)},
            device_id_type=MESH,
        )

    def small_next(bit):
        small_copy(bit).wait_recv()
        return small[bit] + small_recv[bit]

    halo_wait(d_pad, 2)
    small_copy(0).start()

    def conv_back(r, _):
        here = pl.ds(r, ROWS)
        acc = jnp.zeros((ROWS, chans), F32)
        acc = slide(d_pad, r, lambda tap: PAD + reach - tap, acc)
        o = opening[here, :]
        grad = acc * o
        dv[here, :] = grad.astype(BF16)
        dg[here, :] = (grad * value[here, :] * (1.0 - o)).astype(BF16)

    row_loop(conv_back)
    weight_grad(0, x, dv)
    ring_step(0, late[0::2])
    weight_grad(1, x, dg)
    ring_step(0, late[1::2])
    ring_step(2, early)

    half = tokens // 2
    mine = pl.multiple_of(lax.rem(d, 2) * half, half)
    other = pl.multiple_of((1 - lax.rem(d, 2)) * half, half)

    def input_grad(first, target):
        def step(i, _):
            here = pl.ds(pl.multiple_of(i * tile, tile), tile)
            rows = pl.ds(first, half)
            got = dot(dv[rows, :], wv[here, :], NT) + dot(dg[rows, :], wg[here, :], NT)
            target[:, here] = got.astype(target.dtype)

        lax.fori_loop(0, width // tile, step, None)

    def ig_copy(at, src, dst, bit):
        return pltpu.make_async_remote_copy(
            src_ref=src,
            dst_ref=dst,
            send_sem=ig_ssem.at[at],
            recv_sem=ig_rsem.at[at],
            device_id={"dp": flip(d, bit)},
            device_id_type=MESH,
        )

    input_grad(other, ig_send)
    copy0 = ig_copy(0, ig_send, ig_recv, 0)
    copy0.start()
    input_grad(mine, ig_own)
    copy0.wait_recv()

    def wide_loop(fn):
        def step(i, _):
            fn(pl.ds(pl.multiple_of(i * tile, tile), tile))

        lax.fori_loop(0, width // tile, step, None)

    def pair_sum(here):
        ig_sum[0, :, here] = (ig_own[:, here] + ig_recv[:, here].astype(F32)).astype(BF16)

    def y_copy(bit):
        return ig_copy(bit, ig_sum.at[bit - 1], ig_peer.at[bit - 1], bit)

    wide_loop(pair_sum)
    last = bits_dp
    if last > 1:
        y_copy(1).start()
    small[1] = small_next(0)
    if bits_sp > 1:
        small_copy(1).start()

    everything = late + early
    ring_step(1, late)
    ring_step(3, early) if sp > 4 else None
    ring_step(2, late)
    for bit in range(1, bits_sp):
        small[bit + 1] = small_next(bit)
        if bit + 1 < bits_sp:
            small_copy(bit + 1).start()
    ring_step(3, late)

    for_early = 4

    def both(k, _):
        ring_step(k, everything)

    lax.fori_loop(for_early, sp - 2, both, None)

    for bit in range(1, bits_dp):
        y_copy(bit).wait_recv()

        def add(here, bit=bit):
            got = ig_sum[bit - 1, :, here].astype(F32) + ig_peer[bit - 1, :, here].astype(F32)
            ig_sum[bit, :, here] = got.astype(BF16)

        wide_loop(add)
        if bit + 1 < bits_dp:
            y_copy(bit + 1).start()

    final = bits_dp - 1
    give = ig_copy(
        bits_dp, ig_sum.at[final], ig_out.at[pl.ds(mine, half)], 0
    )
    give.start()
    ring_step(sp - 2, everything)

    def keep(here):
        ig_out[pl.ds(mine, half), here] = ig_sum[final, :, here]

    wide_loop(keep)
    small_out[...] = small[bits_sp]
    outs = (vg_out, gg_out, dg_out)
    ring_end(everything, outs)

    copy0.wait_send()
    for bit in range(1, bits_dp):
        y_copy(bit).wait_send()
    give.wait()
    for bit in range(bits_sp):
        small_copy(bit).wait_send()

    def drain(k, _):
        for stream in everything:
            ring_copy(stream, k).wait_send()

    lax.fori_loop(0, sp - 1, drain, None)


def finish(ig, vg, gg, dgrad, small, ig_o, vg_o, gg_o, dg_o, k_o, b_o, g_o, s_o, sem):
    copies = [
        pltpu.make_async_copy(src, dst, sem.at[at])
        for at, (src, dst) in enumerate([(ig, ig_o), (vg, vg_o), (gg, gg_o)])
    ]
    for copy in copies:
        copy.start()
    taps = k_o.shape[0]
    dg_o[...] = dgrad[...].T
    k_o[...] = small[0:taps, :]
    for at, out in enumerate((b_o, g_o, s_o)):
        out[...] = small[taps + at, :]
    for copy in copies:
        copy.wait()


def on_device(
    normed_input,
    out_grad,
    value_weight,
    gate_weight,
    down_weight,
    conv_kernel,
    conv_bias,
    norm_gain,
    norm_shift,
):
    tokens, width = normed_input.shape
    taps, chans = conv_kernel.shape
    sp, dp = lax.axis_size("sp"), lax.axis_size("dp")
    ratio = 1.0 / math.sqrt(tokens * sp)
    chunk = width // sp
    bits_sp, bits_dp = sp.bit_length() - 1, dp.bit_length() - 1
    small_rows = -(-(taps + 3) // 8) * 8
    half = tokens // 2
    full = (tokens, chans)
    vmem = pl.BlockSpec(memory_space=pltpu.VMEM)
    hbm = pl.BlockSpec(memory_space=pltpu.HBM)
    dma = pltpu.SemaphoreType.DMA
    ig, vg, gg, dgrad, small = pl.pallas_call(
        functools.partial(kernel, sp, dp, ratio),
        out_shape=(
            pltpu.VMEM((tokens, width), BF16),
            pltpu.VMEM((chunk, chans), F32),
            pltpu.VMEM((chunk, chans), F32),
            pltpu.VMEM((chunk, chans), F32),
            pltpu.VMEM((small_rows, chans), F32),
        ),
        in_specs=[hbm] * 5 + [vmem] * 4,
        out_specs=(vmem,) * 5,
        scratch_shapes=[
            pltpu.VMEM((tokens, width), BF16),
            pltpu.VMEM((tokens, width), BF16),
            pltpu.VMEM((width, chans), BF16),
            pltpu.VMEM((width, chans), BF16),
            pltpu.VMEM((chans, width), BF16),
            dma((5,)),
            pltpu.VMEM(full, F32),
            pltpu.VMEM(full, F32),
            pltpu.VMEM((tokens + 2 * PAD, chans), F32),
            pltpu.VMEM(full, F32),
            pltpu.VMEM(full, F32),
            pltpu.VMEM((tokens + 2 * PAD, chans), F32),
            pltpu.VMEM(full, BF16),
            pltpu.VMEM(full, BF16),
            pltpu.VMEM(full, BF16),
            pltpu.VMEM((2, tokens, 128), F32),
            pltpu.VMEM((dp, 8, tokens), F32),
            pltpu.VMEM((dp, 8, tokens), F32),
            pltpu.VMEM((3, width, chans), F32),
            pltpu.VMEM((6, sp - 1, chunk // 2, chans), BF16),
            pltpu.VMEM((6, sp - 1, chunk // 2, chans), BF16),
            pltpu.VMEM((half, width), BF16),
            pltpu.VMEM((half, width), BF16),
            pltpu.VMEM((half, width), F32),
            pltpu.VMEM((bits_dp, half, width), BF16),
            pltpu.VMEM((bits_dp - 1, half, width), BF16),
            pltpu.VMEM((bits_sp + 1, small_rows, chans), F32),
            pltpu.VMEM((bits_sp, small_rows, chans), F32),
            dma((4,)),
            dma((4,)),
            dma((2 * dp,)),
            dma((2 * dp,)),
            dma((6, sp - 1)),
            dma((6, sp - 1)),
            dma((bits_dp + 1,)),
            dma((bits_dp + 1,)),
            dma((bits_sp,)),
            dma((bits_sp,)),
        ],
        compiler_params=pltpu.CompilerParams(
            collective_id=0, has_side_effects=True, vmem_limit_bytes=MAIN
        ),
    )(
        normed_input,
        out_grad,
        value_weight,
        gate_weight,
        down_weight,
        conv_kernel,
        conv_bias[None, :],
        norm_gain[None, :],
        norm_shift[None, :],
    )
    row = jax.ShapeDtypeStruct((chans,), F32)
    return pl.pallas_call(
        finish,
        out_shape=(
            jax.ShapeDtypeStruct(ig.shape, BF16),
            jax.ShapeDtypeStruct(vg.shape, F32),
            jax.ShapeDtypeStruct(gg.shape, F32),
            jax.ShapeDtypeStruct((chans, chunk), F32),
            jax.ShapeDtypeStruct((taps, chans), F32),
            row,
            row,
            row,
        ),
        in_specs=[vmem] * 5,
        out_specs=(hbm,) * 3 + (vmem,) * 5,
        scratch_shapes=[dma((3,))],
        compiler_params=pltpu.CompilerParams(vmem_limit_bytes=FINISH),
    )(ig, vg, gg, dgrad, small)


def solution(mesh):
    in_specs = (
        P("sp", None),
        P("sp", None),
        P(None, "dp"),
        P(None, "dp"),
        P("dp", None),
        P(None, "dp"),
        P("dp"),
        P("dp"),
        P("dp"),
    )
    out_specs = (
        P("sp", None),
        P("sp", "dp"),
        P("sp", "dp"),
        P("dp", "sp"),
        P(None, "dp"),
        P("dp"),
        P("dp"),
        P("dp"),
    )
    return jax.shard_map(
        on_device, mesh=mesh, in_specs=in_specs, out_specs=out_specs, check_vma=False
    )
```
